32 devices in a mesh: sp: 8 (over z, x), tp: 4 (over y, core).
Axes of the slice: x: 2, y: 2, z: 4, core: 2. Of those that a mesh axis runs over, the one named last changes fastest.
Arguments:
- tokens: bfloat16 [2048, 4096], P('sp', 'tp'), may hold values from -6 to 6
- norm_gain: float32 [2, 4096], replicated, may hold values from 0.1 to 1.9
- w_value: bfloat16 [2, 4096, 2048], P(None, 'sp', 'tp'), may hold values from -0.09375 to 0.09375
- w_gate: bfloat16 [2, 4096, 2048], P(None, 'sp', 'tp'), may hold values from -0.09375 to 0.09375
- conv_taps: float32 [2, 31, 2048], P(None, None, 'tp'), may hold values from -3 to 3
- conv_bias: float32 [2, 2048], P(None, 'tp'), may hold values from -3 to 3
- chan_gain: float32 [2, 2048], P(None, 'tp'), may hold values from 0.1 to 1.9
- chan_bias: float32 [2, 2048], P(None, 'tp'), may hold values from -3 to 3
- w_out: bfloat16 [2, 2048, 4096], P(None, 'sp', 'tp'), may hold values from -0.125 to 0.125
Outputs:
- stream: bfloat16 [2048, 4096], P('sp', 'tp')
The draws below stay inside these ranges and needn't reach their ends.
All inputs are finite; a program needn't handle non-finite values.
Results may differ from the reference program's by a relative error of at most 0.011.
Values may be sent and summed in bfloat16 or wider, within the bound.
A program may use at most 64 MiB of HBM per device.

```python
import jax
import jax.numpy as jnp
from jax import lax

D = 4096
C = 2048
K = 31
LAYERS = 2
TOKENS = 2048


def draw_conv_taps(key, part):
    first, second = jax.random.split(jax.random.fold_in(key, 7))
    base = jax.random.normal(first, (LAYERS, K, C), jnp.float32)
    factor = jnp.exp(jax.random.uniform(second, (LAYERS, 1, 32), jnp.float32, -1.1, 1.1))
    factor = jnp.repeat(factor, C // 32, axis=2)
    return jnp.clip(base * factor * K ** (-0.5), -3.0, 3.0)


def steps_of(own_key, dims, pieces, low, top_value):
    gain = 1.0
    for axis_at, parts in pieces:
        draws = jax.random.uniform(jax.random.fold_in(jax.random.fold_in(own_key, 6), axis_at), (parts,), jnp.float32, low / len(pieces), top_value / len(pieces))
        gain = gain * jnp.repeat(jnp.exp(draws), dims[axis_at] // parts).reshape((-1,) + (1,) * (len(dims) - 1 - axis_at))
    return gain


def centred(key, shape, scale, reach, pieces=(), kind=jnp.bfloat16):
    drawn = scale * jax.random.normal(key, shape, jnp.float32)
    if pieces:
        drawn = drawn * steps_of(key, shape, pieces, -0.22, 0.18)
    return jnp.clip(drawn, -reach, reach).astype(kind)


def setup_inputs(seed: int = 0) -> dict:
    key_list = jax.random.split(jax.random.key(seed), 10)
    tokens = centred(key_list[0], (TOKENS, D), 1.0, 6.0, ((0, 8), (1, 4)))
    norm_gain = jnp.clip(1.0 + 0.18 * jax.random.normal(key_list[1], (LAYERS, D), jnp.float32), 0.1, 1.9)
    w_value = centred(key_list[2], (LAYERS, D, C), D ** -0.5, 0.09375, ((1, 8), (2, 4)))
    w_gate = centred(key_list[3], (LAYERS, D, C), D ** -0.5, 0.09375, ((1, 8), (2, 4)))
    conv_taps = draw_conv_taps(jax.random.fold_in(key_list[9], 71), 0)
    conv_bias = centred(key_list[5], (LAYERS, C), 0.5, 3.0, ((1, 4),), jnp.float32)
    chan_gain = jnp.clip(1.0 + 0.18 * jax.random.normal(key_list[6], (LAYERS, C), jnp.float32), 0.1, 1.9)
    chan_bias = centred(key_list[7], (LAYERS, C), 0.5, 3.0, ((1, 4),), jnp.float32)
    w_out = centred(key_list[8], (LAYERS, C, D), C ** -0.5, 0.125, ((1, 8), (2, 4)))
    return dict(tokens=tokens, norm_gain=norm_gain, w_value=w_value, w_gate=w_gate, conv_taps=conv_taps, conv_bias=conv_bias, chan_gain=chan_gain, chan_bias=chan_bias, w_out=w_out)


def reference(tokens, norm_gain, w_value, w_gate, conv_taps, conv_bias, chan_gain, chan_bias, w_out):
    stream = tokens
    rows_total = tokens.shape[0]
    for layer_index in range(LAYERS):
        widened = stream.astype(jnp.float32)
        scale = lax.rsqrt(lax.optimization_barrier(jnp.mean(widened * widened, axis=1, keepdims=True)) + 1e-06)
        normed = (widened * scale * norm_gain[layer_index][None, :]).astype(jnp.bfloat16)
        value = jnp.dot(normed, w_value[layer_index], preferred_element_type=jnp.float32)
        gate = jnp.dot(normed, w_gate[layer_index], preferred_element_type=jnp.float32)
        gated = (value * jax.nn.sigmoid(gate)).astype(jnp.bfloat16)
        padded = jnp.pad(gated.astype(jnp.float32), ((K - 1, 0), (0, 0)))
        convolved = jnp.zeros(gated.shape, jnp.float32) + conv_bias[layer_index][None, :]
        for tap_index in range(K):
            convolved = convolved + conv_taps[layer_index, tap_index][None, :] * padded[tap_index:tap_index + rows_total]
        center = lax.optimization_barrier(jnp.mean(convolved, axis=1, keepdims=True))
        meansq = lax.optimization_barrier(jnp.mean(convolved * convolved, axis=1, keepdims=True))
        spread = meansq - center * center
        shaped = (convolved - center) * lax.rsqrt(spread + 1e-05) * chan_gain[layer_index][None, :] + chan_bias[layer_index][None, :]
        activated = jax.nn.silu(shaped).astype(jnp.bfloat16)
        update = jnp.dot(activated, w_out[layer_index], preferred_element_type=jnp.float32)
        stream = (widened + update).astype(jnp.bfloat16)
    return stream
```

```python
import functools

import jax
import jax.numpy as jnp
from jax import lax
from jax.experimental import pallas as pl
from jax.experimental.pallas import tpu as pltpu
from jax.sharding import PartitionSpec as P

LAYERS = 2
MESH = pl.DeviceIdType.MESH


def passed_along(value, axis, steps):
    count = lax.axis_size(axis)
    first, last = (max(0, -steps), min(count, count - steps))
    return lax.ppermute(value, axis, [(source, source + steps) for source in range(first, last)])


def shards(tokens, norm_gain, w_value, w_gate, conv_taps, conv_bias, chan_gain, chan_bias, w_out):
    stream = tokens
    kernel = conv_taps.shape[1]
    channels_all = conv_taps.shape[2] * lax.axis_size("tp")
    rows_here = tokens.shape[0]
    all_value, all_gate, all_out = (
        lax.all_gather(w_value, "sp", axis=1, tiled=True),
        lax.all_gather(w_gate, "sp", axis=1, tiled=True),
        lax.all_gather(w_out, "sp", axis=1, tiled=True),
    )
    for layer_index in range(LAYERS):
        whole = lax.all_gather(stream, "tp", axis=1, tiled=True)
        widened = whole.astype(jnp.float32)
        scale = lax.rsqrt(jnp.mean(widened * widened, axis=1, keepdims=True) + 1e-06)
        normed = (widened * scale * norm_gain[layer_index][None, :]).astype(jnp.bfloat16)
        value = jnp.dot(normed, all_value[layer_index], preferred_element_type=jnp.float32)
        gate = jnp.dot(normed, all_gate[layer_index], preferred_element_type=jnp.float32)
        gated = (value * jax.nn.sigmoid(gate)).astype(jnp.bfloat16)
        earlier = passed_along(gated[rows_here - kernel + 1 :], "sp", 1)
        extended = jnp.concatenate([earlier, gated], axis=0).astype(jnp.float32)
        taps_here = conv_taps[layer_index]
        convolved = jnp.zeros(gated.shape, jnp.float32) + conv_bias[layer_index][None, :]
        for tap_index in range(kernel):
            convolved = (
                convolved
                + taps_here[tap_index][None, :] * extended[tap_index : tap_index + rows_here]
            )
        sum_first, sum_second = lax.psum(
            (jnp.sum(convolved, axis=1), jnp.sum(convolved * convolved, axis=1)), "tp"
        )
        center = (sum_first / channels_all)[:, None]
        meansq = (sum_second / channels_all)[:, None]
        spread = meansq - center * center
        shaped = (convolved - center) * lax.rsqrt(spread + 1e-05) * chan_gain[layer_index][
            None, :
        ] + chan_bias[layer_index][None, :]
        activated = jax.nn.silu(shaped).astype(jnp.bfloat16)
        all_channels = lax.all_gather(activated, "tp", axis=1, tiled=True)
        update = jnp.dot(all_channels, all_out[layer_index], preferred_element_type=jnp.float32)
        stream = (stream.astype(jnp.float32) + update).astype(jnp.bfloat16)
    return stream


def ring_index(place, count):
    side = place // (count // 2)
    return (1 - side) * 2 * place + side * (2 * (count - 1 - place) + 1)


def module_kernel(
    n, t, kernel, tok, gain, wv, wg, taps, cbias, cgain, chbias, wo, out,
    whole, normed, vgbuf, obuf, act, halo, ext, gated, vacc, gacc, oacc, conv, stats,
    w_send, w_recv, t_send, t_recv, h_send, h_recv,
):
    layers = wv.shape[0]
    rows, d_tp = tok.shape
    d_sp, c_tp = wv.shape[1], wv.shape[2]
    c_sp = wo.shape[1]
    half = c_sp // 2
    reach = n // 2
    border = halo.shape[1]
    d_all, c_all = d_tp * t, c_tp * t
    me, my = lax.axis_index("sp"), lax.axis_index("tp")
    z, x = me // 2, me % 2
    pos = z + x * (n - 1 - 2 * z)
    side_at = (ring_index((pos + 1) % n, n), ring_index((pos + n - 1) % n, n))

    def slot(way, hop):
        return hop - 1 if way == 0 or hop == reach else reach + hop - 1

    def sent(l, ph, way, hop, c):
        if ph == 0:
            own = (wv, wg)[c].at[l]
            buf = vgbuf.at[l]
        else:
            own = wo.at[l, pl.ds(c * half, half)]
            buf = obuf.at[l]
        return pltpu.make_async_remote_copy(
            src_ref=own if hop == 1 else buf.at[slot(way, hop - 1), c],
            dst_ref=buf.at[slot(way, hop), c],
            send_sem=w_send.at[l, ph, way, hop - 1, c],
            recv_sem=w_recv.at[l, ph, way, hop - 1, c],
            device_id={"sp": side_at[way]},
            device_id_type=MESH,
        )

    def pieces(hop):
        if hop < reach:
            return [(0, 0), (1, 1), (0, 1), (1, 0)]
        return [(0, 0), (1, 1)]

    def begin(l, ph):
        for way, c in pieces(1):
            sent(l, ph, way, 1, c).start()

    def event(l, ph, hop):
        for way, c in pieces(hop):
            sent(l, ph, way, hop, c).wait_recv()
            if hop < reach and (way, c) in pieces(hop + 1):
                sent(l, ph, way, hop + 1, c).start()

    def sources(hop):
        if hop == reach:
            return [(slot(0, hop), ring_index((pos + n - hop) % n, n))]
        return [
            (slot(0, hop), ring_index((pos + n - hop) % n, n)),
            (slot(1, hop), ring_index((pos + hop) % n, n)),
        ]

    def spread(kind, l, buf):
        found = []
        for d in range(1, t):
            found.append(
                pltpu.make_async_remote_copy(
                    src_ref=buf.at[l, my],
                    dst_ref=buf.at[l, my],
                    send_sem=t_send.at[l, kind, d - 1],
                    recv_sem=t_recv.at[l, kind, d - 1],
                    device_id={"tp": (my + d) % t},
                    device_id_type=MESH,
                )
            )
        return found

    def halo_copy(l):
        return pltpu.make_async_remote_copy(
            src_ref=gated.at[l, pl.ds(rows - border, border)],
            dst_ref=halo.at[l],
            send_sem=h_send.at[l],
            recv_sem=h_recv.at[l],
            device_id={"sp": (me + 1) % n},
            device_id_type=MESH,
        )

    def add_vg(l, source, v_ref, g_ref, first=False):
        block = normed[source]
        v = jnp.dot(block, v_ref[...], preferred_element_type=jnp.float32)
        g = jnp.dot(block, g_ref[...], preferred_element_type=jnp.float32)
        if first:
            vacc[...] = v
            gacc[...] = g
        else:
            vacc[...] += v
            gacc[...] += g

    def add_o(l, source, weight, first=False):
        start = source * c_sp
        block = act[l, start // c_tp, :, pl.ds(pl.multiple_of(start % c_tp, c_sp), c_sp)]
        o = jnp.dot(block, weight, preferred_element_type=jnp.float32)
        if first:
            oacc[...] = o
        else:
            oacc[...] += o

    def norm(l):
        step = 32

        def body(i, _):
            at = pl.ds(pl.multiple_of(i * step, step), step)
            total = jnp.zeros((step, 1), jnp.float32)
            for j in range(t):
                wide = whole[l, j, at, :].astype(jnp.float32)
                total = total + jnp.sum(wide * wide, axis=1, keepdims=True)
            scale = lax.rsqrt(total / d_all + 1e-06)
            for b in range(n):
                j, off = (b * d_sp) // d_tp, (b * d_sp) % d_tp
                wide = whole[l, j, at, off : off + d_sp].astype(jnp.float32)
                g = gain[l : l + 1, b * d_sp : (b + 1) * d_sp]
                normed[b, at, :] = (wide * scale * g).astype(jnp.bfloat16)
            return 0

        lax.fori_loop(0, rows // step, body, 0)

    def gate_up(l):
        gated[l] = (vacc[...] * jax.nn.sigmoid(gacc[...])).astype(jnp.bfloat16)
        ext[border:, :] = gated[l].astype(jnp.float32)

    def convolve(l):
        step = 64
        lane = 128

        def body(i, _):
            base = pl.multiple_of(i * step, step)
            at = pl.ds(base, step)
            first = jnp.zeros((step, lane), jnp.float32)
            second = jnp.zeros((step, lane), jnp.float32)
            for b in range(c_tp // lane):
                cols = slice(b * lane, (b + 1) * lane)
                total = jnp.zeros((step, lane), jnp.float32) + cbias[l : l + 1, cols]
                window = ext[pl.ds(base, step + border), cols]
                for shift in range(8):
                    reads = [
                        (k, border - kernel + 1 + k - shift)
                        for k in range(kernel)
                        if (border - kernel + 1 + k) % 8 == shift
                    ]
                    if not reads:
                        continue
                    top = max(start for _, start in reads) + step
                    moved = window[shift : shift + top]
                    for k, start in reads:
                        total = total + taps[l, k : k + 1, cols] * moved[start : start + step]
                conv[at, cols] = total
                first = first + total
                second = second + total * total
            which = lax.broadcasted_iota(jnp.int32, (step, lane), 1)
            stats[l, my, at, :] = jnp.where(
                which < lane // 2,
                jnp.sum(first, axis=1, keepdims=True),
                jnp.sum(second, axis=1, keepdims=True),
            )
            return 0

        lax.fori_loop(0, rows // step, body, 0)

    def activate(l):
        step = 32

        def body(i, _):
            at = pl.ds(pl.multiple_of(i * step, step), step)
            both = stats[l, 0, at, :]
            for j in range(1, t):
                both = both + stats[l, j, at, :]
            both = both / c_all
            center = both[:, 0:1]
            spread_ = both[:, 64:65] - center * center
            shaped = (conv[at, :] - center) * lax.rsqrt(spread_ + 1e-05) * cgain[
                l : l + 1, :
            ] + chbias[l : l + 1, :]
            act[l, my, at, :] = (shaped * jax.nn.sigmoid(shaped)).astype(jnp.bfloat16)
            return 0

        lax.fori_loop(0, rows // step, body, 0)

    begin(0, 0)
    whole[0, my] = tok[...]
    for copy in spread(0, 0, whole):
        copy.start()
    for l in range(layers):
        if l == 0:
            for copy in spread(0, l, whole):
                copy.wait_recv()
            norm(l)
            event(l, 0, 1)
        else:
            event(l, 0, 1)
            for copy in spread(0, l, whole):
                copy.wait_recv()
            norm(l)
        add_vg(l, me, wv.at[l], wg.at[l], first=True)
        for hop in range(1, reach + 1):
            if hop > 1:
                event(l, 0, hop)
            if hop == reach - 1:
                begin(l, 1)
            for at, source in sources(hop):
                add_vg(l, source, vgbuf.at[l, at, 0], vgbuf.at[l, at, 1])
        gate_up(l)

        @pl.when(me < n - 1)
        def _():
            halo_copy(l).start()

        @pl.when(me > 0)
        def _():
            halo_copy(l).wait_recv()
            ext[0:border, :] = halo[l].astype(jnp.float32)

        @pl.when(me == 0)
        def _():
            ext[0:border, :] = jnp.zeros((border, c_tp), jnp.float32)

        convolve(l)
        for copy in spread(1, l, stats):
            copy.start()
        event(l, 1, 1)
        for copy in spread(1, l, stats):
            copy.wait_recv()
        activate(l)
        for copy in spread(2, l, act):
            copy.start()
        event(l, 1, 2)
        for copy in spread(2, l, act):
            copy.wait_recv()
        add_o(l, me, wo[l], first=True)
        for hop in range(1, reach + 1):
            if hop > 2:
                event(l, 1, hop)
            if hop == reach - 1 and l + 1 < layers:
                begin(l + 1, 0)
            for at, source in sources(hop):
                add_o(l, source, obuf[l, at].reshape(c_sp, d_tp))
        stream = (whole[l, my].astype(jnp.float32) + oacc[...]).astype(jnp.bfloat16)
        if l + 1 < layers:
            whole[l + 1, my] = stream
            for copy in spread(0, l + 1, whole):
                copy.start()
        else:
            out[...] = stream
    for l in range(layers):
        for ph in range(2):
            for hop in range(1, reach + 1):
                for way, c in pieces(hop):
                    sent(l, ph, way, hop, c).wait_send()
        for kind, buf in enumerate((whole, stats, act)):
            for copy in spread(kind, l, buf):
                copy.wait_send()

        @pl.when(me < n - 1)
        def _():
            halo_copy(l).wait_send()


def fused(tokens, norm_gain, w_value, w_gate, conv_taps, conv_bias, chan_gain, chan_bias, w_out):
    n, t = lax.axis_size("sp"), lax.axis_size("tp")
    layers, d_sp, c_tp = w_value.shape
    rows, d_tp = tokens.shape
    c_sp = w_out.shape[1]
    kernel = conv_taps.shape[1]
    border = -(-(kernel - 1) // 16) * 16
    reach = n // 2
    f32, bf16 = jnp.float32, jnp.bfloat16
    vmem = pl.BlockSpec(memory_space=pltpu.VMEM)
    return pl.pallas_call(
        functools.partial(module_kernel, n, t, kernel),
        out_shape=jax.ShapeDtypeStruct((rows, d_tp), bf16),
        in_specs=[vmem] * 9,
        out_specs=vmem,
        scratch_shapes=[
            pltpu.VMEM((layers, t, rows, d_tp), bf16),
            pltpu.VMEM((n, rows, d_sp), bf16),
            pltpu.VMEM((layers, n - 1, 2, d_sp, c_tp), bf16),
            pltpu.VMEM((layers, n - 1, 2, c_sp // 2, d_tp), bf16),
            pltpu.VMEM((layers, t, rows, c_tp), bf16),
            pltpu.VMEM((layers, border, c_tp), bf16),
            pltpu.VMEM((border + rows, c_tp), f32),
            pltpu.VMEM((layers, rows, c_tp), bf16),
            pltpu.VMEM((rows, c_tp), f32),
            pltpu.VMEM((rows, c_tp), f32),
            pltpu.VMEM((rows, d_tp), f32),
            pltpu.VMEM((rows, c_tp), f32),
            pltpu.VMEM((layers, t, rows, 128), f32),
            pltpu.SemaphoreType.DMA((layers, 2, 2, reach, 2)),
            pltpu.SemaphoreType.DMA((layers, 2, 2, reach, 2)),
            pltpu.SemaphoreType.DMA((layers, 3, t - 1)),
            pltpu.SemaphoreType.DMA((layers, 3, t - 1)),
            pltpu.SemaphoreType.DMA((layers,)),
            pltpu.SemaphoreType.DMA((layers,)),
        ],
        compiler_params=pltpu.CompilerParams(
            has_side_effects=True, vmem_limit_bytes=60 * 1024 * 1024
        ),
    )(tokens, norm_gain, w_value, w_gate, conv_taps, conv_bias, chan_gain, chan_bias, w_out)


def fits(n, t, tokens, w_value, conv_taps, w_out):
    d_sp, c_tp = w_value.shape[1:]
    rows, d_tp = tokens.shape
    c_sp = w_out.shape[1]
    return (
        n % 2 == 0
        and n >= 4
        and t >= 2
        and d_sp % 128 == 0
        and d_tp % d_sp == 0
        and c_sp % 128 == 0
        and c_tp % c_sp == 0
        and rows % 64 == 0
        and conv_taps.shape[1] <= rows
    )


def local(tokens, norm_gain, w_value, w_gate, conv_taps, conv_bias, chan_gain, chan_bias, w_out):
    args = (tokens, norm_gain, w_value, w_gate, conv_taps, conv_bias, chan_gain, chan_bias, w_out)
    n, t = lax.axis_size("sp"), lax.axis_size("tp")
    if fits(n, t, tokens, w_value, conv_taps, w_out):
        return fused(*args)
    return shards(*args)


def solution(mesh):
    placed = (
        P("sp", "tp"),
        P(),
        P(None, "sp", "tp"),
        P(None, "sp", "tp"),
        P(None, None, "tp"),
        P(None, "tp"),
        P(None, "tp"),
        P(None, "tp"),
        P(None, "sp", "tp"),
    )
    return jax.shard_map(
        local, mesh=mesh, in_specs=placed, out_specs=P("sp", "tp"), check_vma=False
    )
```

```python
import functools

import jax
import jax.numpy as jnp
from jax import lax
from jax.experimental import pallas as pl
from jax.experimental.pallas import tpu as pltpu
from jax.sharding import PartitionSpec as P

LAYERS = 2
MESH = pl.DeviceIdType.MESH


def passed_along(value, axis, steps):
    count = lax.axis_size(axis)
    first, last = (max(0, -steps), min(count, count - steps))
    return lax.ppermute(value, axis, [(source, source + steps) for source in range(first, last)])


def shards(tokens, norm_gain, w_value, w_gate, conv_taps, conv_bias, chan_gain, chan_bias, w_out):
    stream = tokens
    kernel = conv_taps.shape[1]
    channels_all = conv_taps.shape[2] * lax.axis_size("tp")
    rows_here = tokens.shape[0]
    all_value, all_gate, all_out = (
        lax.all_gather(w_value, "sp", axis=1, tiled=True),
        lax.all_gather(w_gate, "sp", axis=1, tiled=True),
        lax.all_gather(w_out, "sp", axis=1, tiled=True),
    )
    for layer_index in range(LAYERS):
        whole = lax.all_gather(stream, "tp", axis=1, tiled=True)
        widened = whole.astype(jnp.float32)
        scale = lax.rsqrt(jnp.mean(widened * widened, axis=1, keepdims=True) + 1e-06)
        normed = (widened * scale * norm_gain[layer_index][None, :]).astype(jnp.bfloat16)
        value = jnp.dot(normed, all_value[layer_index], preferred_element_type=jnp.float32)
        gate = jnp.dot(normed, all_gate[layer_index], preferred_element_type=jnp.float32)
        gated = (value * jax.nn.sigmoid(gate)).astype(jnp.bfloat16)
        earlier = passed_along(gated[rows_here - kernel + 1 :], "sp", 1)
        extended = jnp.concatenate([earlier, gated], axis=0).astype(jnp.float32)
        taps_here = conv_taps[layer_index]
        convolved = jnp.zeros(gated.shape, jnp.float32) + conv_bias[layer_index][None, :]
        for tap_index in range(kernel):
            convolved = (
                convolved
                + taps_here[tap_index][None, :] * extended[tap_index : tap_index + rows_here]
            )
        sum_first, sum_second = lax.psum(
            (jnp.sum(convolved, axis=1), jnp.sum(convolved * convolved, axis=1)), "tp"
        )
        center = (sum_first / channels_all)[:, None]
        meansq = (sum_second / channels_all)[:, None]
        spread = meansq - center * center
        shaped = (convolved - center) * lax.rsqrt(spread + 1e-05) * chan_gain[layer_index][
            None, :
        ] + chan_bias[layer_index][None, :]
        activated = jax.nn.silu(shaped).astype(jnp.bfloat16)
        all_channels = lax.all_gather(activated, "tp", axis=1, tiled=True)
        update = jnp.dot(all_channels, all_out[layer_index], preferred_element_type=jnp.float32)
        stream = (stream.astype(jnp.float32) + update).astype(jnp.bfloat16)
    return stream


def ring_index(place, count):
    side = place // (count // 2)
    return (1 - side) * 2 * place + side * (2 * (count - 1 - place) + 1)


def module_kernel(
    n, t, kernel, tok, gain, wv_far, wg_far, taps, cbias, cgain, chbias, wo_far, out,
    whole, normed, vgbuf, obuf, act, halo, ext, gated, vacc, gacc, oacc, conv, stats,
    wv, wg, wo, scaled, blocks, sums_out, sums_in, squares,
    w_send, w_recv, t_send, t_recv, h_send, h_recv,
    l_sem, a_send, a_recv, s_send, s_recv, r_send, r_recv,
):
    layers = wv.shape[0]
    rows, d_tp = tok.shape
    d_sp, c_tp = wv.shape[1], wv.shape[2]
    c_sp = wo.shape[1]
    half = c_sp // 2
    reach = n // 2
    border = halo.shape[1]
    d_all, c_all = d_tp * t, c_tp * t
    me, my = lax.axis_index("sp"), lax.axis_index("tp")
    z, x = me // 2, me % 2
    pos = z + x * (n - 1 - 2 * z)
    side_at = (ring_index((pos + 1) % n, n), ring_index((pos + n - 1) % n, n))

    def slot(way, hop):
        return hop - 1 if way == 0 or hop == reach else reach + hop - 1

    def sent(l, ph, way, hop, c):
        if ph == 0:
            own = (wv_far, wg_far)[c].at[l]
            buf = vgbuf.at[l - 1]
        else:
            own = wo_far.at[l, pl.ds(c * half, half)]
            buf = obuf.at[l]
        return pltpu.make_async_remote_copy(
            src_ref=own if hop == 1 else buf.at[slot(way, hop - 1), c],
            dst_ref=buf.at[slot(way, hop), c],
            send_sem=w_send.at[l, ph, way, hop - 1, c],
            recv_sem=w_recv.at[l, ph, way, hop - 1, c],
            device_id={"sp": side_at[way]},
            device_id_type=MESH,
        )

    def pieces(hop):
        if hop < reach:
            return [(0, 0), (1, 1), (0, 1), (1, 0)]
        return [(0, 0), (1, 1)]

    def begin(l, ph):
        for way, c in pieces(1):
            sent(l, ph, way, 1, c).start()

    def event(l, ph, hop):
        for way, c in pieces(hop):
            sent(l, ph, way, hop, c).wait_recv()
            if hop < reach and (way, c) in pieces(hop + 1):
                sent(l, ph, way, hop + 1, c).start()

    def sources(hop):
        if hop == reach:
            return [(slot(0, hop), ring_index((pos + n - hop) % n, n))]
        return [
            (slot(0, hop), ring_index((pos + n - hop) % n, n)),
            (slot(1, hop), ring_index((pos + hop) % n, n)),
        ]

    def spread(kind, l, buf):
        found = []
        for d in range(1, t):
            found.append(
                pltpu.make_async_remote_copy(
                    src_ref=buf.at[l, my],
                    dst_ref=buf.at[l, my],
                    send_sem=t_send.at[l, kind, d - 1],
                    recv_sem=t_recv.at[l, kind, d - 1],
                    device_id={"tp": (my + d) % t},
                    device_id_type=MESH,
                )
            )
        return found

    def halo_copy(l):
        return pltpu.make_async_remote_copy(
            src_ref=gated.at[l, pl.ds(rows - border, border)],
            dst_ref=halo.at[l],
            send_sem=h_send.at[l],
            recv_sem=h_recv.at[l],
            device_id={"sp": (me + 1) % n},
            device_id_type=MESH,
        )

    def add_vg(l, source, v_ref, g_ref, first=False):
        block = normed[source]
        v = jnp.dot(block, v_ref[...], preferred_element_type=jnp.float32)
        g = jnp.dot(block, g_ref[...], preferred_element_type=jnp.float32)
        if first:
            vacc[...] = v
            gacc[...] = g
        else:
            vacc[...] += v
            gacc[...] += g

    def add_o(l, source, weight, first=False):
        start = source * c_sp
        block = act[l, start // c_tp, :, pl.ds(pl.multiple_of(start % c_tp, c_sp), c_sp)]
        o = jnp.dot(block, weight, preferred_element_type=jnp.float32)
        if first:
            oacc[...] = o
        else:
            oacc[...] += o

    def norm(l):
        step = 32

        def body(i, _):
            at = pl.ds(pl.multiple_of(i * step, step), step)
            total = jnp.zeros((step, 1), jnp.float32)
            for j in range(t):
                wide = whole[l, j, at, :].astype(jnp.float32)
                total = total + jnp.sum(wide * wide, axis=1, keepdims=True)
            scale = lax.rsqrt(total / d_all + 1e-06)
            for b in range(n):
                j, off = (b * d_sp) // d_tp, (b * d_sp) % d_tp
                wide = whole[l, j, at, off : off + d_sp].astype(jnp.float32)
                g = gain[l : l + 1, b * d_sp : (b + 1) * d_sp]
                normed[b, at, :] = (wide * scale * g).astype(jnp.bfloat16)
            return 0

        lax.fori_loop(0, rows // step, body, 0)

    def gate_up(l):
        value, gate = vacc[...], gacc[...]
        if l == 0:
            total = squares[0, 0]
            for j in range(1, t):
                total = total + squares[0, j]
            scale = lax.rsqrt(total[:, 0:1] / d_all + 1e-06)
            value, gate = value * scale, gate * scale
        gated[l] = (value * jax.nn.sigmoid(gate)).astype(jnp.bfloat16)
        ext[border:, :] = gated[l].astype(jnp.float32)

    def convolve(l):
        step = 64
        lane = 128

        def body(i, _):
            base = pl.multiple_of(i * step, step)
            at = pl.ds(base, step)
            first = jnp.zeros((step, lane), jnp.float32)
            second = jnp.zeros((step, lane), jnp.float32)
            for b in range(c_tp // lane):
                cols = slice(b * lane, (b + 1) * lane)
                total = jnp.zeros((step, lane), jnp.float32) + cbias[l : l + 1, cols]
                window = ext[pl.ds(base, step + border), cols]
                for shift in range(8):
                    reads = [
                        (k, border - kernel + 1 + k - shift)
                        for k in range(kernel)
                        if (border - kernel + 1 + k) % 8 == shift
                    ]
                    if not reads:
                        continue
                    top = max(start for _, start in reads) + step
                    moved = window[shift : shift + top]
                    for k, start in reads:
                        total = total + taps[l, k : k + 1, cols] * moved[start : start + step]
                conv[at, cols] = total
                first = first + total
                second = second + total * total
            which = lax.broadcasted_iota(jnp.int32, (step, lane), 1)
            stats[l, my, at, :] = jnp.where(
                which < lane // 2,
                jnp.sum(first, axis=1, keepdims=True),
                jnp.sum(second, axis=1, keepdims=True),
            )
            return 0

        lax.fori_loop(0, rows // step, body, 0)

    def activate(l):
        step = 32

        def body(i, _):
            at = pl.ds(pl.multiple_of(i * step, step), step)
            both = stats[l, 0, at, :]
            for j in range(1, t):
                both = both + stats[l, j, at, :]
            both = both / c_all
            center = both[:, 0:1]
            spread_ = both[:, 64:65] - center * center
            shaped = (conv[at, :] - center) * lax.rsqrt(spread_ + 1e-05) * cgain[
                l : l + 1, :
            ] + chbias[l : l + 1, :]
            act[l, my, at, :] = (shaped * jax.nn.sigmoid(shaped)).astype(jnp.bfloat16)
            return 0

        lax.fori_loop(0, rows // step, body, 0)

    per = d_tp // d_sp
    part = rows // t
    mine = pl.ds(pl.multiple_of(my * part, part), part)

    def around(off):
        return ring_index((pos + off + n) % n, n)

    def local_copies():
        pairs = ((wv_far, wv), (wg_far, wg), (wo_far, wo))
        return [pltpu.make_async_copy(a, b, l_sem.at[i]) for i, (a, b) in enumerate(pairs)]

    def deal(u, q):
        return pltpu.make_async_remote_copy(
            src_ref=scaled.at[u, pl.ds(q * part, part)],
            dst_ref=blocks.at[me, pl.ds(q * part, part)],
            send_sem=a_send.at[u, q],
            recv_sem=a_recv.at[me],
            device_id={"sp": my * per + u, "tp": q},
            device_id_type=MESH,
        )

    def dealt(source):
        return pltpu.make_async_remote_copy(
            src_ref=scaled.at[0, mine],
            dst_ref=blocks.at[source, mine],
            send_sem=a_send.at[0, 0],
            recv_sem=a_recv.at[source],
            device_id={"sp": source, "tp": my},
            device_id_type=MESH,
        )

    def share(source, d):
        return pltpu.make_async_remote_copy(
            src_ref=blocks.at[source, mine],
            dst_ref=blocks.at[source, mine],
            send_sem=s_send.at[source, d - 1],
            recv_sem=s_recv.at[source, d - 1],
            device_id={"tp": (my + d) % t},
            device_id_type=MESH,
        )

    def shared(source):
        for d in range(1, t):
            pltpu.make_async_remote_copy(
                src_ref=blocks.at[source, mine],
                dst_ref=blocks.at[
                    source, pl.ds(pl.multiple_of(((my + t - d) % t) * part, part), part)
                ],
                send_sem=s_send.at[source, d - 1],
                recv_sem=s_recv.at[source, d - 1],
                device_id={"tp": (my + d) % t},
                device_id_type=MESH,
            ).wait_recv()

    def passed(way, d, c):
        return pltpu.make_async_remote_copy(
            src_ref=sums_out.at[way, d - 1, c],
            dst_ref=sums_in.at[way, d - 1, c],
            send_sem=r_send.at[way, d - 1, c],
            recv_sem=r_recv.at[way, d - 1, c],
            device_id={"sp": side_at[way]},
            device_id_type=MESH,
        )

    def travels(way, d, c):
        return d < reach or (d == reach and c == way)

    def reduce_step(d):
        for way in range(2):
            source = around(d if way == 0 else -d)
            if d < reach or way == 0:
                shared(source)
            for c in (way, 1 - way):
                if not travels(way, d, c):
                    continue
                total = jnp.dot(
                    blocks[source], (wv, wg)[c][0], preferred_element_type=jnp.float32
                )
                if d < reach and travels(way, d + 1, c):
                    passed(way, d + 1, c).wait_recv()
                    total = total + sums_in[way, d, c].astype(jnp.float32)
                sums_out[way, d - 1, c] = total.astype(jnp.bfloat16)
                passed(way, d, c).start()

    def for_dealt(action):
        for u in range(per):
            for q in range(t):

                @pl.when(jnp.logical_or(my * per + u != me, my != q))
                def _():
                    action(deal(u, q))

    for copy in local_copies():
        copy.start()
    at_home = my == me // per

    for u in range(per):
        scaled[u] = (
            tok[:, u * d_sp : (u + 1) * d_sp].astype(jnp.float32)
            * gain[pl.ds(0, 1), pl.ds(pl.multiple_of((my * per + u) * d_sp, d_sp), d_sp)]
        ).astype(jnp.bfloat16)
    for_dealt(lambda copy: copy.start())

    @pl.when(at_home)
    def _():
        blocks[me, mine] = scaled[me % per, mine]

    begin(0, 1)
    wide = tok[...].astype(jnp.float32)
    squares[0, my] = jnp.broadcast_to(
        jnp.sum(wide * wide, axis=1, keepdims=True), (rows, squares.shape[3])
    )
    for copy in spread(3, 0, squares):
        copy.start()
    whole[0, my] = tok[...]
    order = [reach] + [o for d in range(reach - 1, 0, -1) for o in (d, -d)] + [0]
    for off in order:
        source = around(off)
        if off == 0:

            @pl.when(jnp.logical_not(at_home))
            def _():
                dealt(source).wait_recv()

        else:
            dealt(source).wait_recv()
        for d in range(1, t):
            share(source, d).start()
    event(0, 1, 1)
    for copy in local_copies():
        copy.wait()
    for d in range(reach, 0, -1):
        reduce_step(d)
        if d > 1:
            event(0, 1, reach - d + 2)
    begin(1, 0)
    shared(me)
    for c, acc in enumerate((vacc, gacc)):
        acc[...] = jnp.dot(blocks[me], (wv, wg)[c][0], preferred_element_type=jnp.float32)
        for way in range(2):
            passed(way, 1, c).wait_recv()
            acc[...] += sums_in[way, 0, c].astype(jnp.float32)
    for copy in spread(3, 0, squares):
        copy.wait_recv()

    for l in range(layers):
        if l > 0:
            if l > 1:
                event(l, 0, 1)
                event(l, 0, 2)
            for copy in spread(0, l, whole):
                copy.wait_recv()
            norm(l)
            add_vg(l, me, wv.at[l], wg.at[l], first=True)
            for hop in range(1, reach + 1):
                if hop > 2:
                    event(l, 0, hop)
                if hop == max(2, reach - 1):
                    begin(l, 1)
                for at, source in sources(hop):
                    add_vg(l, source, vgbuf.at[l - 1, at, 0], vgbuf.at[l - 1, at, 1])
        gate_up(l)

        @pl.when(me < n - 1)
        def _():
            halo_copy(l).start()

        @pl.when(me > 0)
        def _():
            halo_copy(l).wait_recv()
            ext[0:border, :] = halo[l].astype(jnp.float32)

        @pl.when(me == 0)
        def _():
            ext[0:border, :] = jnp.zeros((border, c_tp), jnp.float32)

        convolve(l)
        for copy in spread(1, l, stats):
            copy.start()
        if l > 0:
            event(l, 1, 1)
        for copy in spread(1, l, stats):
            copy.wait_recv()
        activate(l)
        for copy in spread(2, l, act):
            copy.start()
        if l > 0:
            event(l, 1, 2)
        elif layers > 1:
            event(1, 0, 1)
        for copy in spread(2, l, act):
            copy.wait_recv()
        add_o(l, me, wo[l], first=True)
        for hop in range(1, reach + 1):
            if l > 0 and hop > 2:
                event(l, 1, hop)
            if l > 0 and hop == max(2, reach - 1) and l + 1 < layers:
                begin(l + 1, 0)
            for at, source in sources(hop):
                add_o(l, source, obuf[l, at].reshape(c_sp, d_tp))
        stream = (whole[l, my].astype(jnp.float32) + oacc[...]).astype(jnp.bfloat16)
        if l + 1 < layers:
            whole[l + 1, my] = stream
            for copy in spread(0, l + 1, whole):
                copy.start()
            if l == 0:
                event(1, 0, 2)
        else:
            out[...] = stream
    for_dealt(lambda copy: copy.wait_send())
    for source in range(n):
        for d in range(1, t):
            share(source, d).wait_send()
    for d in range(1, reach + 1):
        for way in range(2):
            for c in range(2):
                if travels(way, d, c):
                    passed(way, d, c).wait_send()
    for copy in spread(3, 0, squares):
        copy.wait_send()
    for l in range(layers):
        for ph in range(2):
            if (l, ph) == (0, 0):
                continue
            for hop in range(1, reach + 1):
                for way, c in pieces(hop):
                    sent(l, ph, way, hop, c).wait_send()
        for kind, buf in enumerate((whole, stats, act)):
            if (l, kind) == (0, 0):
                continue
            for copy in spread(kind, l, buf):
                copy.wait_send()

        @pl.when(me < n - 1)
        def _():
            halo_copy(l).wait_send()


def fused(tokens, norm_gain, w_value, w_gate, conv_taps, conv_bias, chan_gain, chan_bias, w_out):
    n, t = lax.axis_size("sp"), lax.axis_size("tp")
    layers, d_sp, c_tp = w_value.shape
    rows, d_tp = tokens.shape
    c_sp = w_out.shape[1]
    kernel = conv_taps.shape[1]
    border = -(-(kernel - 1) // 16) * 16
    reach = n // 2
    f32, bf16 = jnp.float32, jnp.bfloat16
    vmem = pl.BlockSpec(memory_space=pltpu.VMEM)
    far = pl.BlockSpec(memory_space=pl.ANY)
    return pl.pallas_call(
        functools.partial(module_kernel, n, t, kernel),
        out_shape=jax.ShapeDtypeStruct((rows, d_tp), bf16),
        in_specs=[vmem, vmem, far, far, vmem, vmem, vmem, vmem, far],
        out_specs=vmem,
        scratch_shapes=[
            pltpu.VMEM((layers, t, rows, d_tp), bf16),
            pltpu.VMEM((n, rows, d_sp), bf16),
            pltpu.VMEM((layers - 1, n - 1, 2, d_sp, c_tp), bf16),
            pltpu.VMEM((layers, n - 1, 2, c_sp // 2, d_tp), bf16),
            pltpu.VMEM((layers, t, rows, c_tp), bf16),
            pltpu.VMEM((layers, border, c_tp), bf16),
            pltpu.VMEM((border + rows, c_tp), f32),
            pltpu.VMEM((layers, rows, c_tp), bf16),
            pltpu.VMEM((rows, c_tp), f32),
            pltpu.VMEM((rows, c_tp), f32),
            pltpu.VMEM((rows, d_tp), f32),
            pltpu.VMEM((rows, c_tp), f32),
            pltpu.VMEM((layers, t, rows, 128), f32),
            pltpu.VMEM((layers, d_sp, c_tp), bf16),
            pltpu.VMEM((layers, d_sp, c_tp), bf16),
            pltpu.VMEM((layers, c_sp, d_tp), bf16),
            pltpu.VMEM((d_tp // d_sp, rows, d_sp), bf16),
            pltpu.VMEM((n, rows, d_sp), bf16),
            pltpu.VMEM((2, reach, 2, rows, c_tp), bf16),
            pltpu.VMEM((2, reach, 2, rows, c_tp), bf16),
            pltpu.VMEM((1, t, rows, 128), f32),
            pltpu.SemaphoreType.DMA((layers, 2, 2, reach, 2)),
            pltpu.SemaphoreType.DMA((layers, 2, 2, reach, 2)),
            pltpu.SemaphoreType.DMA((layers, 4, t - 1)),
            pltpu.SemaphoreType.DMA((layers, 4, t - 1)),
            pltpu.SemaphoreType.DMA((layers,)),
            pltpu.SemaphoreType.DMA((layers,)),
            pltpu.SemaphoreType.DMA((3,)),
            pltpu.SemaphoreType.DMA((d_tp // d_sp, t)),
            pltpu.SemaphoreType.DMA((n,)),
            pltpu.SemaphoreType.DMA((n, t - 1)),
            pltpu.SemaphoreType.DMA((n, t - 1)),
            pltpu.SemaphoreType.DMA((2, reach, 2)),
            pltpu.SemaphoreType.DMA((2, reach, 2)),
        ],
        compiler_params=pltpu.CompilerParams(
            has_side_effects=True, vmem_limit_bytes=60 * 1024 * 1024
        ),
    )(tokens, norm_gain, w_value, w_gate, conv_taps, conv_bias, chan_gain, chan_bias, w_out)


def fits(n, t, tokens, w_value, conv_taps, w_out):
    d_sp, c_tp = w_value.shape[1:]
    rows, d_tp = tokens.shape
    c_sp = w_out.shape[1]
    return (
        n % 2 == 0
        and n >= 4
        and t >= 2
        and d_sp % 128 == 0
        and d_tp % d_sp == 0
        and c_sp % 128 == 0
        and c_tp % c_sp == 0
        and rows % 64 == 0
        and rows % (16 * t) == 0
        and w_value.shape[0] >= 2
        and conv_taps.shape[1] <= rows
    )


def local(tokens, norm_gain, w_value, w_gate, conv_taps, conv_bias, chan_gain, chan_bias, w_out):
    args = (tokens, norm_gain, w_value, w_gate, conv_taps, conv_bias, chan_gain, chan_bias, w_out)
    n, t = lax.axis_size("sp"), lax.axis_size("tp")
    if fits(n, t, tokens, w_value, conv_taps, w_out):
        return fused(*args)
    return shards(*args)


def solution(mesh):
    placed = (
        P("sp", "tp"),
        P(),
        P(None, "sp", "tp"),
        P(None, "sp", "tp"),
        P(None, None, "tp"),
        P(None, "tp"),
        P(None, "tp"),
        P(None, "tp"),
        P(None, "sp", "tp"),
    )
    return jax.shard_map(
        local, mesh=mesh, in_specs=placed, out_specs=P("sp", "tp"), check_vma=False
    )
```

```python
import functools

import jax
import jax.numpy as jnp
from jax import lax
from jax.experimental import pallas as pl
from jax.experimental.pallas import tpu as pltpu
from jax.sharding import PartitionSpec as P

LAYERS = 2
MESH = pl.DeviceIdType.MESH


def passed_along(value, axis, steps):
    count = lax.axis_size(axis)
    first, last = (max(0, -steps), min(count, count - steps))
    return lax.ppermute(value, axis, [(source, source + steps) for source in range(first, last)])


def shards(tokens, norm_gain, w_value, w_gate, conv_taps, conv_bias, chan_gain, chan_bias, w_out):
    stream = tokens
    kernel = conv_taps.shape[1]
    channels_all = conv_taps.shape[2] * lax.axis_size("tp")
    rows_here = tokens.shape[0]
    all_value, all_gate, all_out = (
        lax.all_gather(w_value, "sp", axis=1, tiled=True),
        lax.all_gather(w_gate, "sp", axis=1, tiled=True),
        lax.all_gather(w_out, "sp", axis=1, tiled=True),
    )
    for layer_index in range(LAYERS):
        whole = lax.all_gather(stream, "tp", axis=1, tiled=True)
        widened = whole.astype(jnp.float32)
        scale = lax.rsqrt(jnp.mean(widened * widened, axis=1, keepdims=True) + 1e-06)
        normed = (widened * scale * norm_gain[layer_index][None, :]).astype(jnp.bfloat16)
        value = jnp.dot(normed, all_value[layer_index], preferred_element_type=jnp.float32)
        gate = jnp.dot(normed, all_gate[layer_index], preferred_element_type=jnp.float32)
        gated = (value * jax.nn.sigmoid(gate)).astype(jnp.bfloat16)
        earlier = passed_along(gated[rows_here - kernel + 1 :], "sp", 1)
        extended = jnp.concatenate([earlier, gated], axis=0).astype(jnp.float32)
        taps_here = conv_taps[layer_index]
        convolved = jnp.zeros(gated.shape, jnp.float32) + conv_bias[layer_index][None, :]
        for tap_index in range(kernel):
            convolved = (
                convolved
                + taps_here[tap_index][None, :] * extended[tap_index : tap_index + rows_here]
            )
        sum_first, sum_second = lax.psum(
            (jnp.sum(convolved, axis=1), jnp.sum(convolved * convolved, axis=1)), "tp"
        )
        center = (sum_first / channels_all)[:, None]
        meansq = (sum_second / channels_all)[:, None]
        spread = meansq - center * center
        shaped = (convolved - center) * lax.rsqrt(spread + 1e-05) * chan_gain[layer_index][
            None, :
        ] + chan_bias[layer_index][None, :]
        activated = jax.nn.silu(shaped).astype(jnp.bfloat16)
        all_channels = lax.all_gather(activated, "tp", axis=1, tiled=True)
        update = jnp.dot(all_channels, all_out[layer_index], preferred_element_type=jnp.float32)
        stream = (stream.astype(jnp.float32) + update).astype(jnp.bfloat16)
    return stream


def ring_index(place, count):
    side = place // (count // 2)
    return (1 - side) * 2 * place + side * (2 * (count - 1 - place) + 1)


def module_kernel(
    n, t, kernel, tok, gain, wv_far, wg_far, taps, cbias, cgain, chbias, wo_far, out,
    whole, normed, vgbuf, obuf, act, halo, ext, gated, vacc, gacc, oacc, conv, stats,
    wv, wg, wo, scaled, blocks, sums_out, sums_in, squares,
    w_send, w_recv, t_send, t_recv, h_send, h_recv,
    l_sem, a_send, a_recv, s_send, s_recv, r_send, r_recv,
):
    layers = wv.shape[0]
    rows, d_tp = tok.shape
    d_sp, c_tp = wv.shape[1], wv.shape[2]
    c_sp = wo.shape[1]
    half = c_sp // 2
    reach = n // 2
    border = halo.shape[1]
    d_all, c_all = d_tp * t, c_tp * t
    me, my = lax.axis_index("sp"), lax.axis_index("tp")
    z, x = me // 2, me % 2
    pos = z + x * (n - 1 - 2 * z)
    side_at = (ring_index((pos + 1) % n, n), ring_index((pos + n - 1) % n, n))

    def slot(way, hop):
        return hop - 1 if way == 0 or hop == reach else reach + hop - 1

    def sent(l, ph, way, hop, c):
        if ph == 0:
            own = (wv_far, wg_far)[c].at[l]
            buf = vgbuf.at[l - 1]
        else:
            own = wo_far.at[l, pl.ds(c * half, half)]
            buf = obuf.at[l]
        return pltpu.make_async_remote_copy(
            src_ref=own if hop == 1 else buf.at[slot(way, hop - 1), c],
            dst_ref=buf.at[slot(way, hop), c],
            send_sem=w_send.at[l, ph, way, hop - 1, c],
            recv_sem=w_recv.at[l, ph, way, hop - 1, c],
            device_id={"sp": side_at[way]},
            device_id_type=MESH,
        )

    def pieces(hop):
        if hop < reach:
            return [(0, 0), (1, 1), (0, 1), (1, 0)]
        return [(0, 0), (1, 1)]

    def begin(l, ph):
        for way, c in pieces(1):
            sent(l, ph, way, 1, c).start()

    def event(l, ph, hop):
        for way, c in pieces(hop):
            sent(l, ph, way, hop, c).wait_recv()
            if hop < reach and (way, c) in pieces(hop + 1):
                sent(l, ph, way, hop + 1, c).start()

    def sources(hop):
        if hop == reach:
            return [(slot(0, hop), ring_index((pos + n - hop) % n, n))]
        return [
            (slot(0, hop), ring_index((pos + n - hop) % n, n)),
            (slot(1, hop), ring_index((pos + hop) % n, n)),
        ]

    def spread(kind, l, buf):
        found = []
        for d in range(1, t):
            found.append(
                pltpu.make_async_remote_copy(
                    src_ref=buf.at[l, my],
                    dst_ref=buf.at[l, my],
                    send_sem=t_send.at[l, kind, d - 1],
                    recv_sem=t_recv.at[l, kind, d - 1],
                    device_id={"tp": (my + d) % t},
                    device_id_type=MESH,
                )
            )
        return found

    def halo_copy(l):
        return pltpu.make_async_remote_copy(
            src_ref=gated.at[l, pl.ds(rows - border, border)],
            dst_ref=halo.at[l],
            send_sem=h_send.at[l],
            recv_sem=h_recv.at[l],
            device_id={"sp": (me + 1) % n},
            device_id_type=MESH,
        )

    def add_vg(l, source, v_ref, g_ref, first=False):
        block = normed[source]
        v = jnp.dot(block, v_ref[...], preferred_element_type=jnp.float32)
        g = jnp.dot(block, g_ref[...], preferred_element_type=jnp.float32)
        if first:
            vacc[...] = v
            gacc[...] = g
        else:
            vacc[...] += v
            gacc[...] += g

    def add_o(l, source, weight, first=False):
        start = source * c_sp
        block = act[l, start // c_tp, :, pl.ds(pl.multiple_of(start % c_tp, c_sp), c_sp)]
        o = jnp.dot(block, weight, preferred_element_type=jnp.float32)
        if first:
            oacc[...] = o
        else:
            oacc[...] += o

    def norm(l):
        step = 32

        def body(i, _):
            at = pl.ds(pl.multiple_of(i * step, step), step)
            total = jnp.zeros((step, 1), jnp.float32)
            for j in range(t):
                wide = whole[l, j, at, :].astype(jnp.float32)
                total = total + jnp.sum(wide * wide, axis=1, keepdims=True)
            scale = lax.rsqrt(total / d_all + 1e-06)
            for b in range(n):
                j, off = (b * d_sp) // d_tp, (b * d_sp) % d_tp
                wide = whole[l, j, at, off : off + d_sp].astype(jnp.float32)
                g = gain[l : l + 1, b * d_sp : (b + 1) * d_sp]
                normed[b, at, :] = (wide * scale * g).astype(jnp.bfloat16)
            return 0

        lax.fori_loop(0, rows // step, body, 0)

    def gate_up(l):
        value, gate = vacc[...], gacc[...]
        if l == 0:
            total = squares[0, 0]
            for j in range(1, t):
                total = total + squares[0, j]
            scale = lax.rsqrt(total[:, 0:1] / d_all + 1e-06)
            value, gate = value * scale, gate * scale
        gated[l] = (value * jax.nn.sigmoid(gate)).astype(jnp.bfloat16)
        ext[border:, :] = gated[l].astype(jnp.float32)

    def convolve(l):
        step = 64
        lane = 128

        def body(i, _):
            base = pl.multiple_of(i * step, step)
            at = pl.ds(base, step)
            first = jnp.zeros((step, lane), jnp.float32)
            second = jnp.zeros((step, lane), jnp.float32)
            for b in range(c_tp // lane):
                cols = slice(b * lane, (b + 1) * lane)
                total = jnp.zeros((step, lane), jnp.float32) + cbias[l : l + 1, cols]
                window = ext[pl.ds(base, step + border), cols]
                for shift in range(8):
                    reads = [
                        (k, border - kernel + 1 + k - shift)
                        for k in range(kernel)
                        if (border - kernel + 1 + k) % 8 == shift
                    ]
                    if not reads:
                        continue
                    top = max(start for _, start in reads) + step
                    moved = window[shift : shift + top]
                    for k, start in reads:
                        total = total + taps[l, k : k + 1, cols] * moved[start : start + step]
                conv[at, cols] = total
                first = first + total
                second = second + total * total
            which = lax.broadcasted_iota(jnp.int32, (step, lane), 1)
            stats[l, my, at, :] = jnp.where(
                which < lane // 2,
                jnp.sum(first, axis=1, keepdims=True),
                jnp.sum(second, axis=1, keepdims=True),
            )
            return 0

        lax.fori_loop(0, rows // step, body, 0)

    def activate(l):
        step = 32

        def body(i, _):
            at = pl.ds(pl.multiple_of(i * step, step), step)
            both = stats[l, 0, at, :]
            for j in range(1, t):
                both = both + stats[l, j, at, :]
            both = both / c_all
            center = both[:, 0:1]
            spread_ = both[:, 64:65] - center * center
            shaped = (conv[at, :] - center) * lax.rsqrt(spread_ + 1e-05) * cgain[
                l : l + 1, :
            ] + chbias[l : l + 1, :]
            act[l, my, at, :] = (shaped * jax.nn.sigmoid(shaped)).astype(jnp.bfloat16)
            return 0

        lax.fori_loop(0, rows // step, body, 0)

    per = d_tp // d_sp
    part = rows // t
    mine = pl.ds(pl.multiple_of(my * part, part), part)

    def around(off):
        return ring_index((pos + off + n) % n, n)

    def local_copies():
        pairs = ((wv_far, wv), (wg_far, wg), (wo_far, wo))
        return [pltpu.make_async_copy(a, b, l_sem.at[i]) for i, (a, b) in enumerate(pairs)]

    def deal(u, q):
        return pltpu.make_async_remote_copy(
            src_ref=scaled.at[u, pl.ds(q * part, part)],
            dst_ref=blocks.at[me, pl.ds(q * part, part)],
            send_sem=a_send.at[u, q],
            recv_sem=a_recv.at[me],
            device_id={"sp": my * per + u, "tp": q},
            device_id_type=MESH,
        )

    def dealt(source):
        return pltpu.make_async_remote_copy(
            src_ref=scaled.at[0, mine],
            dst_ref=blocks.at[source, mine],
            send_sem=a_send.at[0, 0],
            recv_sem=a_recv.at[source],
            device_id={"sp": source, "tp": my},
            device_id_type=MESH,
        )

    def share(source, d):
        return pltpu.make_async_remote_copy(
            src_ref=blocks.at[source, mine],
            dst_ref=blocks.at[source, mine],
            send_sem=s_send.at[source, d - 1],
            recv_sem=s_recv.at[source, d - 1],
            device_id={"tp": (my + d) % t},
            device_id_type=MESH,
        )

    def shared(source):
        for d in range(1, t):
            pltpu.make_async_remote_copy(
                src_ref=blocks.at[source, mine],
                dst_ref=blocks.at[
                    source, pl.ds(pl.multiple_of(((my + t - d) % t) * part, part), part)
                ],
                send_sem=s_send.at[source, d - 1],
                recv_sem=s_recv.at[source, d - 1],
                device_id={"tp": (my + d) % t},
                device_id_type=MESH,
            ).wait_recv()

    def passed(way, d, c):
        return pltpu.make_async_remote_copy(
            src_ref=sums_out.at[way, d - 1, c],
            dst_ref=sums_in.at[way, d - 1, c],
            send_sem=r_send.at[way, d - 1, c],
            recv_sem=r_recv.at[way, d - 1, c],
            device_id={"sp": side_at[way]},
            device_id_type=MESH,
        )

    def travels(way, d, c):
        return d < reach or (d == reach and c == way)

    def reduce_step(d):
        for way in range(2):
            source = around(d if way == 0 else -d)
            if d < reach or way == 0:
                shared(source)
            for c in (way, 1 - way):
                if not travels(way, d, c):
                    continue
                total = jnp.dot(
                    blocks[source], (wv, wg)[c][0], preferred_element_type=jnp.float32
                )
                if d < reach and travels(way, d + 1, c):
                    passed(way, d + 1, c).wait_recv()
                    total = total + sums_in[way, d, c].astype(jnp.float32)
                sums_out[way, d - 1, c] = total.astype(jnp.bfloat16)
                passed(way, d, c).start()

    def for_dealt(action):
        for u in range(per):
            for q in range(t):

                @pl.when(jnp.logical_or(my * per + u != me, my != q))
                def _():
                    action(deal(u, q))

    for copy in local_copies():
        copy.start()
    at_home = my == me // per

    def greet(sp, tp):
        pl.semaphore_signal(
            barrier, inc=1, device_id={"sp": sp, "tp": tp}, device_id_type=MESH
        )

    barrier = pltpu.get_barrier_semaphore()
    for sp in (side_at[0], side_at[1], (me + n - 1) % n):
        greet(sp, my)
    for d in range(1, t):
        greet(me, (my + d) % t)
    for i in range(1, n):
        greet((me + i) % n, me // per)

    @pl.when(jnp.logical_not(at_home))
    def _():
        greet(me, me // per)
        pl.semaphore_wait(barrier, 2 + t + n)

    @pl.when(at_home)
    def _():
        pl.semaphore_wait(barrier, 1 + t + n)

    for u in range(per):
        scaled[u] = (
            tok[:, u * d_sp : (u + 1) * d_sp].astype(jnp.float32)
            * gain[pl.ds(0, 1), pl.ds(pl.multiple_of((my * per + u) * d_sp, d_sp), d_sp)]
        ).astype(jnp.bfloat16)
    for_dealt(lambda copy: copy.start())

    @pl.when(at_home)
    def _():
        blocks[me, mine] = scaled[me % per, mine]

    begin(0, 1)
    wide = tok[...].astype(jnp.float32)
    squares[0, my] = jnp.broadcast_to(
        jnp.sum(wide * wide, axis=1, keepdims=True), (rows, squares.shape[3])
    )
    for copy in spread(3, 0, squares):
        copy.start()
    whole[0, my] = tok[...]
    order = [reach] + [o for d in range(reach - 1, 0, -1) for o in (d, -d)] + [0]
    for off in order:
        source = around(off)
        if off == 0:

            @pl.when(jnp.logical_not(at_home))
            def _():
                dealt(source).wait_recv()

        else:
            dealt(source).wait_recv()
        for d in range(1, t):
            share(source, d).start()
    event(0, 1, 1)
    for copy in local_copies():
        copy.wait()
    for d in range(reach, 0, -1):
        reduce_step(d)
        if d > 1:
            event(0, 1, reach - d + 2)
    begin(1, 0)
    shared(me)
    for c, acc in enumerate((vacc, gacc)):
        acc[...] = jnp.dot(blocks[me], (wv, wg)[c][0], preferred_element_type=jnp.float32)
        for way in range(2):
            passed(way, 1, c).wait_recv()
            acc[...] += sums_in[way, 0, c].astype(jnp.float32)
    for copy in spread(3, 0, squares):
        copy.wait_recv()

    for l in range(layers):
        if l > 0:
            if l > 1:
                event(l, 0, 1)
                event(l, 0, 2)
            for copy in spread(0, l, whole):
                copy.wait_recv()
            norm(l)
            add_vg(l, me, wv.at[l], wg.at[l], first=True)
            for hop in range(1, reach + 1):
                if hop > 2:
                    event(l, 0, hop)
                if hop == max(2, reach - 1):
                    begin(l, 1)
                for at, source in sources(hop):
                    add_vg(l, source, vgbuf.at[l - 1, at, 0], vgbuf.at[l - 1, at, 1])
        gate_up(l)

        @pl.when(me < n - 1)
        def _():
            halo_copy(l).start()

        @pl.when(me > 0)
        def _():
            halo_copy(l).wait_recv()
            ext[0:border, :] = halo[l].astype(jnp.float32)

        @pl.when(me == 0)
        def _():
            ext[0:border, :] = jnp.zeros((border, c_tp), jnp.float32)

        convolve(l)
        for copy in spread(1, l, stats):
            copy.start()
        if l > 0:
            event(l, 1, 1)
        elif layers > 1:
            event(1, 0, 1)
        for copy in spread(1, l, stats):
            copy.wait_recv()
        activate(l)
        for copy in spread(2, l, act):
            copy.start()
        if l > 0:
            event(l, 1, 2)
        for copy in spread(2, l, act):
            copy.wait_recv()
        add_o(l, me, wo[l], first=True)
        for hop in range(1, reach + 1):
            if l > 0 and hop > 2:
                event(l, 1, hop)
            if l > 0 and hop == max(2, reach - 1) and l + 1 < layers:
                begin(l + 1, 0)
            for at, source in sources(hop):
                add_o(l, source, obuf[l, at].reshape(c_sp, d_tp))
        stream = (whole[l, my].astype(jnp.float32) + oacc[...]).astype(jnp.bfloat16)
        if l + 1 < layers:
            whole[l + 1, my] = stream
            for copy in spread(0, l + 1, whole):
                copy.start()
            if l == 0:
                event(1, 0, 2)
        else:
            out[...] = stream
    for_dealt(lambda copy: copy.wait_send())
    for source in range(n):
        for d in range(1, t):
            share(source, d).wait_send()
    for d in range(1, reach + 1):
        for way in range(2):
            for c in range(2):
                if travels(way, d, c):
                    passed(way, d, c).wait_send()
    for copy in spread(3, 0, squares):
        copy.wait_send()
    for l in range(layers):
        for ph in range(2):
            if (l, ph) == (0, 0):
                continue
            for hop in range(1, reach + 1):
                for way, c in pieces(hop):
                    sent(l, ph, way, hop, c).wait_send()
        for kind, buf in enumerate((whole, stats, act)):
            if (l, kind) == (0, 0):
                continue
            for copy in spread(kind, l, buf):
                copy.wait_send()

        @pl.when(me < n - 1)
        def _():
            halo_copy(l).wait_send()


def fused(tokens, norm_gain, w_value, w_gate, conv_taps, conv_bias, chan_gain, chan_bias, w_out):
    n, t = lax.axis_size("sp"), lax.axis_size("tp")
    layers, d_sp, c_tp = w_value.shape
    rows, d_tp = tokens.shape
    c_sp = w_out.shape[1]
    kernel = conv_taps.shape[1]
    border = -(-(kernel - 1) // 16) * 16
    reach = n // 2
    f32, bf16 = jnp.float32, jnp.bfloat16
    vmem = pl.BlockSpec(memory_space=pltpu.VMEM)
    far = pl.BlockSpec(memory_space=pl.ANY)
    return pl.pallas_call(
        functools.partial(module_kernel, n, t, kernel),
        out_shape=jax.ShapeDtypeStruct((rows, d_tp), bf16),
        in_specs=[vmem, vmem, far, far, vmem, vmem, vmem, vmem, far],
        out_specs=vmem,
        scratch_shapes=[
            pltpu.VMEM((layers, t, rows, d_tp), bf16),
            pltpu.VMEM((n, rows, d_sp), bf16),
            pltpu.VMEM((layers - 1, n - 1, 2, d_sp, c_tp), bf16),
            pltpu.VMEM((layers, n - 1, 2, c_sp // 2, d_tp), bf16),
            pltpu.VMEM((layers, t, rows, c_tp), bf16),
            pltpu.VMEM((layers, border, c_tp), bf16),
            pltpu.VMEM((border + rows, c_tp), f32),
            pltpu.VMEM((layers, rows, c_tp), bf16),
            pltpu.VMEM((rows, c_tp), f32),
            pltpu.VMEM((rows, c_tp), f32),
            pltpu.VMEM((rows, d_tp), f32),
            pltpu.VMEM((rows, c_tp), f32),
            pltpu.VMEM((layers, t, rows, 128), f32),
            pltpu.VMEM((layers, d_sp, c_tp), bf16),
            pltpu.VMEM((layers, d_sp, c_tp), bf16),
            pltpu.VMEM((layers, c_sp, d_tp), bf16),
            pltpu.VMEM((d_tp // d_sp, rows, d_sp), bf16),
            pltpu.VMEM((n, rows, d_sp), bf16),
            pltpu.VMEM((2, reach, 2, rows, c_tp), bf16),
            pltpu.VMEM((2, reach, 2, rows, c_tp), bf16),
            pltpu.VMEM((1, t, rows, 128), f32),
            pltpu.SemaphoreType.DMA((layers, 2, 2, reach, 2)),
            pltpu.SemaphoreType.DMA((layers, 2, 2, reach, 2)),
            pltpu.SemaphoreType.DMA((layers, 4, t - 1)),
            pltpu.SemaphoreType.DMA((layers, 4, t - 1)),
            pltpu.SemaphoreType.DMA((layers,)),
            pltpu.SemaphoreType.DMA((layers,)),
            pltpu.SemaphoreType.DMA((3,)),
            pltpu.SemaphoreType.DMA((d_tp // d_sp, t)),
            pltpu.SemaphoreType.DMA((n,)),
            pltpu.SemaphoreType.DMA((n, t - 1)),
            pltpu.SemaphoreType.DMA((n, t - 1)),
            pltpu.SemaphoreType.DMA((2, reach, 2)),
            pltpu.SemaphoreType.DMA((2, reach, 2)),
        ],
        compiler_params=pltpu.CompilerParams(
            has_side_effects=True, collective_id=0, vmem_limit_bytes=60 * 1024 * 1024
        ),
    )(tokens, norm_gain, w_value, w_gate, conv_taps, conv_bias, chan_gain, chan_bias, w_out)


def fits(n, t, tokens, w_value, conv_taps, w_out):
    d_sp, c_tp = w_value.shape[1:]
    rows, d_tp = tokens.shape
    c_sp = w_out.shape[1]
    return (
        n % 2 == 0
        and n >= 4
        and t >= 2
        and d_sp % 128 == 0
        and d_tp % d_sp == 0
        and c_sp % 128 == 0
        and c_tp % c_sp == 0
        and rows % 64 == 0
        and rows % (16 * t) == 0
        and w_value.shape[0] >= 2
        and conv_taps.shape[1] <= rows
    )


def local(tokens, norm_gain, w_value, w_gate, conv_taps, conv_bias, chan_gain, chan_bias, w_out):
    args = (tokens, norm_gain, w_value, w_gate, conv_taps, conv_bias, chan_gain, chan_bias, w_out)
    n, t = lax.axis_size("sp"), lax.axis_size("tp")
    if fits(n, t, tokens, w_value, conv_taps, w_out):
        return fused(*args)
    return shards(*args)


def solution(mesh):
    placed = (
        P("sp", "tp"),
        P(),
        P(None, "sp", "tp"),
        P(None, "sp", "tp"),
        P(None, None, "tp"),
        P(None, "tp"),
        P(None, "tp"),
        P(None, "tp"),
        P(None, "sp", "tp"),
    )
    return jax.shard_map(
        local, mesh=mesh, in_specs=placed, out_specs=P("sp", "tp"), check_vma=False
    )
```
